32 devices in a mesh: grp: 2 (over y), fs: 4 (over z), tp: 4 (over x, core).
Axes of the slice: x: 2, y: 2, z: 4, core: 2. Of those that a mesh axis runs over, the one named last changes fastest.
Arguments:
- tokens: bfloat16 [8192, 2048], P(('grp', 'fs'), 'tp'), parts along dimension 0, may hold values from -6 to 6
- norm1_gain: float32 [2048], replicated, may hold values from 0.1 to 1.9
- weight_u: float32 [2048, 1024], P('fs', 'tp'), may hold values from -0.125 to 0.125
- weight_v: float32 [2048, 1024], P('fs', 'tp'), may hold values from -0.125 to 0.125
- scale_u: float32 [1024], P('tp'), may hold values from 0.5 to 2
- scale_v: float32 [1024], P('tp'), may hold values from 0.05 to 4.5
- mix_gain: float32 [1024], P('tp'), may hold values from 0.1 to 1.9
- spatial_weight: float32 [4, 128, 128], replicated, may hold values from -0.5 to 0.5
- spatial_bias: float32 [4, 128], replicated, may hold values from 0.5 to 1.5
- weight_out: float32 [1024, 2048], P('tp', 'fs'), may hold values from -0.1875 to 0.1875
- scale_out: float32 [2048], P('fs'), may hold values from 0.5 to 2
- norm2_gain: float32 [2048], replicated, may hold values from 0.1 to 1.9
- weight_up: float32 [2048, 8192], P('fs', 'tp'), may hold values from -0.125 to 0.125
- scale_up: float32 [8192], P('tp'), may hold values from 0.5 to 2
- weight_down: float32 [8192, 2048], P('tp', 'fs'), may hold values from -0.0625 to 0.0625
- scale_down: float32 [2048], P('fs'), may hold values from 0.5 to 2
Outputs:
- result: bfloat16 [8192, 2048], P(('grp', 'fs'), 'tp'), parts along dimension 0
The draws below stay inside these ranges and needn't reach their ends.
There are 2 independent parts, one for each index of `grp`. The reference program is written for one: setup_inputs(seed, part) draws one part's arguments, and reference() takes and returns one part's arrays. A program takes and returns all parts, laid end to end along the dimension named above; an argument that names none is the same for every part. Nothing has to cross between parts.
All inputs are finite; a program needn't handle non-finite values.
Results may differ from the reference program's by a relative error of at most 0.023.
Values may be sent and summed in bfloat16 or wider, within the bound.
A program may use at most 128 MiB of HBM per device.

```python
import math
import jax
import jax.numpy as jnp
from jax import lax

D = 2048
GM_W = 1024
GROUPS = 4
BLOCK = 128
FF = 8192
TOKENS = 4096
N_TP = 4


def draw_scale_v(key, part):
    columns = jnp.arange(GM_W, dtype=jnp.float32) / GM_W
    roughness = jax.random.uniform(key, (GM_W,), jnp.float32, 0.5, 1.5)
    return 0.4 * jnp.exp(columns * jnp.log(4.0)) * roughness


def level_of(stream_key, dims, split, least, top_value):
    gain, own = 1.0, jax.random.fold_in(stream_key, 6)
    for axis_at, blocks in split:
        heights = jnp.exp(jax.random.uniform(jax.random.fold_in(own, axis_at), (blocks,), jnp.float32, least / len(split), top_value / len(split)))
        gain = gain * jnp.repeat(heights, dims[axis_at] // blocks).reshape([-1 if axis == axis_at else 1 for axis in range(len(dims))])
    return gain


def bell_draw(stream_key, dims, spread, limit, cuts=(), kind=jnp.bfloat16):
    entries = spread * jax.random.normal(stream_key, dims, jnp.float32)
    if cuts:
        entries = entries * level_of(stream_key, dims, cuts, -0.22, 0.18)
    return jnp.clip(entries, -limit, limit).astype(kind)


def setup_inputs(seed: int = 0, part: int = 0) -> dict:
    seeds = jax.random.split(jax.random.key(seed), 17)
    part_keys = jax.random.split(jax.random.fold_in(seeds[16], part), 17)
    tokens = bell_draw(part_keys[0], (TOKENS, D), 1.0, 6.0, ((0, 4), (1, 4)))
    norm1_gain = jnp.clip(1.0 + 0.18 * jax.random.normal(seeds[1], (D,), jnp.float32), 0.1, 1.9)
    weight_u = bell_draw(seeds[2], (D, GM_W), D ** -0.5, 0.125, ((0, 4), (1, 4)), jnp.float32)
    weight_v = bell_draw(seeds[3], (D, GM_W), D ** -0.5, 0.125, ((0, 4), (1, 4)), jnp.float32)
    scale_u = jnp.clip(jnp.exp(math.log(2.0) - 1.3862944 * jax.random.uniform(seeds[4], (GM_W,), jnp.float32) ** level_of(seeds[4], (GM_W,), ((0, 4),), -0.2, 0.2)), 0.5, 2.0)
    scale_v = draw_scale_v(jax.random.fold_in(seeds[16], 71), part)
    mix_gain = jnp.clip(1.0 + 0.18 * jax.random.normal(seeds[6], (GM_W,), jnp.float32), 0.1, 1.9)
    spatial_weight = bell_draw(seeds[7], (GROUPS, BLOCK, BLOCK), BLOCK ** -0.5, 0.5, (), jnp.float32)
    spatial_bias = jnp.clip(jax.random.uniform(seeds[8], (GROUPS, BLOCK), jnp.float32, 0.5, 1.5), 0.5, 1.5)
    weight_out = bell_draw(seeds[9], (GM_W, D), GM_W ** -0.5, 0.1875, ((0, 4), (1, 4)), jnp.float32)
    scale_out = jnp.clip(jnp.exp(math.log(2.0) - 1.3862944 * jax.random.uniform(seeds[10], (D,), jnp.float32) ** level_of(seeds[10], (D,), ((0, 4),), -0.2, 0.2)), 0.5, 2.0)
    norm2_gain = jnp.clip(1.0 + 0.18 * jax.random.normal(seeds[11], (D,), jnp.float32), 0.1, 1.9)
    weight_up = bell_draw(seeds[12], (D, FF), D ** -0.5, 0.125, ((0, 4), (1, 4)), jnp.float32)
    scale_up = jnp.clip(jnp.exp(math.log(2.0) - 1.3862944 * jax.random.uniform(seeds[13], (FF,), jnp.float32) ** level_of(seeds[13], (FF,), ((0, 4),), -0.2, 0.2)), 0.5, 2.0)
    weight_down = bell_draw(seeds[14], (FF, D), FF ** -0.5, 0.0625, ((0, 4), (1, 4)), jnp.float32)
    scale_down = jnp.clip(jnp.exp(math.log(2.0) - 1.3862944 * jax.random.uniform(seeds[15], (D,), jnp.float32) ** level_of(seeds[15], (D,), ((0, 4),), -0.2, 0.2)), 0.5, 2.0)
    return {"tokens": tokens, "norm1_gain": norm1_gain, "weight_u": weight_u, "weight_v": weight_v, "scale_u": scale_u, "scale_v": scale_v, "mix_gain": mix_gain, "spatial_weight": spatial_weight, "spatial_bias": spatial_bias, "weight_out": weight_out, "scale_out": scale_out, "norm2_gain": norm2_gain, "weight_up": weight_up, "scale_up": scale_up, "weight_down": weight_down, "scale_down": scale_down}


def rms_rows(values, gain_vector):
    widened = values.astype(jnp.float32)
    scaled = widened * lax.rsqrt(lax.optimization_barrier(jnp.mean(widened * widened, axis=-1, keepdims=True)) + 1e-06)
    return (scaled * gain_vector).astype(jnp.bfloat16)

def run_sum(operand_left, operand_right, column_scale, pieces):
    run_width = operand_left.shape[1] // pieces
    running = jnp.zeros((operand_left.shape[0], operand_right.shape[1]), jnp.float32)
    for run_index in range(pieces):
        lower = run_index * run_width
        partial_term = jnp.dot(operand_left[:, lower:lower + run_width], operand_right[lower:lower + run_width], preferred_element_type=jnp.float32) * column_scale
        running = running + lax.optimization_barrier(partial_term.astype(jnp.bfloat16)).astype(jnp.float32)
    return running

def reference(tokens, norm1_gain, weight_u, weight_v, scale_u, scale_v, mix_gain, spatial_weight, spatial_bias, weight_out, scale_out, norm2_gain, weight_up, scale_up, weight_down, scale_down):
    normed_in = rms_rows(tokens, norm1_gain)
    pre_u = jnp.dot(normed_in, weight_u.astype(jnp.bfloat16), preferred_element_type=jnp.float32) * scale_u
    pre_v = jnp.dot(normed_in, weight_v.astype(jnp.bfloat16), preferred_element_type=jnp.float32) * scale_v
    gate_u = jax.nn.gelu(pre_u)
    act_v = jax.nn.gelu(pre_v)
    row_mean = lax.optimization_barrier(jnp.mean(act_v, axis=-1, keepdims=True))
    square = lax.optimization_barrier(jnp.mean(act_v * act_v, axis=-1, keepdims=True))
    v_norm = ((act_v - row_mean) * lax.rsqrt(square - row_mean * row_mean + 1e-06) * mix_gain).astype(jnp.bfloat16)
    lower_mask = jnp.tril(jnp.ones((BLOCK, BLOCK), jnp.float32))
    spatial_mask = (spatial_weight * lower_mask).astype(jnp.bfloat16)
    blocks = v_norm.reshape(TOKENS // BLOCK, BLOCK, GROUPS, GM_W // GROUPS)
    mixed_cols = jnp.einsum('gts,nsgc->ntgc', spatial_mask.astype(jnp.float32), blocks.astype(jnp.float32))
    mixed_cols = mixed_cols + spatial_bias.T[None, :, :, None]
    gated = (gate_u * mixed_cols.reshape(TOKENS, GM_W)).astype(jnp.bfloat16)
    mixer_sum = run_sum(gated, weight_out.astype(jnp.bfloat16), scale_out, N_TP)
    residual = (tokens.astype(jnp.float32) + mixer_sum).astype(jnp.bfloat16)
    normed_mid = rms_rows(residual, norm2_gain)
    pre_up = jnp.dot(normed_mid, weight_up.astype(jnp.bfloat16), preferred_element_type=jnp.float32) * scale_up
    hidden = jnp.square(jax.nn.relu(pre_up)).astype(jnp.bfloat16)
    channel_sum = run_sum(hidden, weight_down.astype(jnp.bfloat16), scale_down, N_TP)
    return (residual.astype(jnp.float32) + channel_sum).astype(jnp.bfloat16)
```

```python
import jax
import jax.numpy as jnp
from jax import lax
from jax.sharding import PartitionSpec as P

GM_W = 1024
GROUPS = 4
BLOCK = 128


def swap(value, axis, size, mask):
    return lax.ppermute(value, axis, [(k, k ^ mask) for k in range(size)])


def over_fs(piece, fs):
    if fs != 4:
        return [piece] + [swap(piece, "fs", fs, mask) for mask in range(1, fs)]
    far = swap(piece, "fs", 4, 2)
    near = swap(piece, "fs", 4, 1)
    middle = lax.ppermute(piece, "fs", [(1, 2), (2, 1)])
    relayed = lax.ppermute(far, "fs", [(1, 0), (2, 3)])
    me = lax.axis_index("fs")
    last = jnp.where((me == 1) | (me == 2), middle, relayed)
    return [piece, near, far, last]


def gather_weight(shard, cut_axis, fs):
    half = shard.shape[cut_axis] // 2
    group = lax.axis_index("grp")
    mine = lax.dynamic_slice_in_dim(shard, group * half, half, cut_axis)
    other = lax.dynamic_slice_in_dim(shard, (1 - group) * half, half, cut_axis)
    firsts = over_fs(mine, fs)
    seconds = [other] + [
        lax.ppermute(firsts[mask], "grp", [(0, 1), (1, 0)]) for mask in range(1, fs)
    ]
    return firsts, seconds


def halves_swapped(value, axis):
    half = value.shape[axis] // 2
    group = lax.axis_index("grp")
    return jnp.concatenate(
        [
            lax.dynamic_slice_in_dim(value, group * half, half, axis),
            lax.dynamic_slice_in_dim(value, (1 - group) * half, half, axis),
        ],
        axis=axis,
    )


def gather_rows(piece, tp):
    blocks = [None] * tp
    blocks[0] = piece
    bit = tp // 2
    while bit:
        for at in range(tp):
            if blocks[at] is not None and not at & bit and blocks[at | bit] is None:
                blocks[at | bit] = "due"
        for at in range(tp):
            if isinstance(blocks[at], str):
                blocks[at] = swap(blocks[at ^ bit], "tp", tp, bit)
        bit //= 2
    return blocks


def normed_blocks(blocks, gain, fs, tp):
    feature_count = gain.shape[0]
    width, fine = feature_count // tp, feature_count // fs
    squares = sum(
        jnp.sum(jnp.square(block.astype(jnp.float32)), axis=1) for block in blocks
    )
    inverse = lax.rsqrt(squares / feature_count + 1e-06)[:, None]
    stacked = jnp.stack(blocks)
    me_fs, me_tp = lax.axis_index("fs"), lax.axis_index("tp")
    pieces = []
    for mask in range(fs):
        block = me_fs ^ mask
        first = block * fine
        whole = lax.dynamic_index_in_dim(stacked, (first // width) ^ me_tp, 0, keepdims=False)
        if fine != width:
            whole = lax.dynamic_slice_in_dim(whole, first % width, fine, 1)
        gain_piece = lax.dynamic_slice_in_dim(gain, first, fine, 0)
        pieces.append((whole.astype(jnp.float32) * inverse * gain_piece).astype(jnp.bfloat16))
    return jnp.concatenate(pieces, axis=1)


def scatter_sum(terms, fs, tp):
    stacked = jnp.stack(terms)
    ratio = fs // tp
    me_fs, me_tp = lax.axis_index("fs"), lax.axis_index("tp")
    sums = []
    for mask in range(tp):
        parts = [
            lax.dynamic_index_in_dim(
                stacked, ((me_tp ^ mask) * ratio + at) ^ me_fs, 0, keepdims=False
            )
            for at in range(ratio)
        ]
        sums.append(parts[0] if ratio == 1 else jnp.concatenate(parts, axis=1))
    bit = 1
    while bit < tp:
        kept = {}
        for at in range(tp):
            if sums[at] is not None and not at & bit:
                got = swap(sums[at | bit].astype(jnp.bfloat16), "tp", tp, bit)
                kept[at] = sums[at].astype(jnp.float32) + got.astype(jnp.float32)
        sums = [kept.get(at) for at in range(tp)]
        bit *= 2
    return sums[0]


def make(fs, tp):
    def layer(
        tokens,
        norm1_gain,
        weight_u,
        weight_v,
        scale_u,
        scale_v,
        mix_gain,
        spatial_weight,
        spatial_bias,
        weight_out,
        scale_out,
        norm2_gain,
        weight_up,
        scale_up,
        weight_down,
        scale_down,
    ):
        half = weight_u.shape[1] // 2
        token_blocks = gather_rows(tokens, tp)
        both = jnp.stack([weight_u, weight_v], axis=1).astype(jnp.bfloat16)
        both_mine, both_other = gather_weight(both, 2, fs)
        scales = jnp.stack([scale_out, scale_down])
        all_scales = [scales] + [swap(scales, "fs", fs, mask) for mask in range(1, fs)]
        out_mine, out_other = gather_weight(weight_out.astype(jnp.bfloat16), 0, fs)
        up_mine, up_other = gather_weight(weight_up.astype(jnp.bfloat16), 1, fs)
        down_mine, down_other = gather_weight(weight_down.astype(jnp.bfloat16), 0, fs)

        normed_in = normed_blocks(token_blocks, norm1_gain, fs, tp)
        full_u = jnp.concatenate(
            [jnp.concatenate([a[:, 0], b[:, 0]], axis=1) for a, b in zip(both_mine, both_other)]
        )
        full_v = jnp.concatenate(
            [jnp.concatenate([a[:, 1], b[:, 1]], axis=1) for a, b in zip(both_mine, both_other)]
        )
        pre_v = jnp.dot(normed_in, full_v, preferred_element_type=jnp.float32)
        pre_u = jnp.dot(normed_in, full_u, preferred_element_type=jnp.float32)
        act_v = jax.nn.gelu(pre_v * halves_swapped(scale_v, 0))
        gate_u = jax.nn.gelu(pre_u * halves_swapped(scale_u, 0))
        local_width = 2 * half
        row_sums, row_squares = lax.psum(
            (jnp.sum(act_v, axis=1), jnp.sum(act_v * act_v, axis=1)), "tp"
        )
        row_mean = (row_sums / GM_W)[:, None]
        square = (row_squares / GM_W)[:, None]
        v_norm = (
            (act_v - row_mean)
            * lax.rsqrt(square - row_mean * row_mean + 1e-06)
            * halves_swapped(mix_gain, 0)
        ).astype(jnp.bfloat16)
        group_index = lax.axis_index("tp") * local_width // (GM_W // GROUPS)
        lower_mask = jnp.tril(jnp.ones((BLOCK, BLOCK), jnp.float32))
        spatial_mask = (
            lax.dynamic_index_in_dim(spatial_weight, group_index, 0, keepdims=False) * lower_mask
        ).astype(jnp.bfloat16)
        block_bias = lax.dynamic_index_in_dim(spatial_bias, group_index, 0, keepdims=False)
        blocks = v_norm.reshape(-1, BLOCK, local_width)
        mixed = jnp.einsum("ts,nsc->ntc", spatial_mask, blocks, preferred_element_type=jnp.float32)
        mixed = mixed + block_bias[None, :, None]
        gated = (gate_u * mixed.reshape(-1, local_width)).astype(jnp.bfloat16)

        terms = []
        for a, b, scale in zip(out_mine, out_other, all_scales):
            product = jnp.dot(gated, jnp.concatenate([a, b]), preferred_element_type=jnp.float32)
            terms.append((product * scale[0]).astype(jnp.bfloat16))
        mixer_sum = scatter_sum(terms, fs, tp)
        residual = (tokens.astype(jnp.float32) + mixer_sum).astype(jnp.bfloat16)

        normed_mid = normed_blocks(gather_rows(residual, tp), norm2_gain, fs, tp)
        full_up = jnp.concatenate(
            [jnp.concatenate([a, b], axis=1) for a, b in zip(up_mine, up_other)]
        )
        pre_up = jnp.dot(normed_mid, full_up, preferred_element_type=jnp.float32)
        hidden = jnp.square(jax.nn.relu(pre_up * halves_swapped(scale_up, 0))).astype(jnp.bfloat16)
        terms = []
        for a, b, scale in zip(down_mine, down_other, all_scales):
            product = jnp.dot(hidden, jnp.concatenate([a, b]), preferred_element_type=jnp.float32)
            terms.append((product * scale[1]).astype(jnp.bfloat16))
        channel_sum = scatter_sum(terms, fs, tp)
        return (residual.astype(jnp.float32) + channel_sum).astype(jnp.bfloat16)

    return layer


def solution(mesh):
    placed = (
        P(("grp", "fs"), "tp"),
        P(),
        P("fs", "tp"),
        P("fs", "tp"),
        P("tp"),
        P("tp"),
        P("tp"),
        P(),
        P(),
        P("tp", "fs"),
        P("fs"),
        P(),
        P("fs", "tp"),
        P("tp"),
        P("tp", "fs"),
        P("fs"),
    )
    fs, tp = mesh.shape["fs"], mesh.shape["tp"]
    return jax.shard_map(
        make(fs, tp),
        mesh=mesh,
        in_specs=placed,
        out_specs=P(("grp", "fs"), "tp"),
        check_vma=False,
    )
```

```python
import jax
import jax.numpy as jnp
from jax import lax
from jax.sharding import PartitionSpec as P

GM_W = 1024
GROUPS = 4
BLOCK = 128


def swap(value, axis, size, mask):
    return lax.ppermute(value, axis, [(k, k ^ mask) for k in range(size)])


def over_fs(piece, fs, relay):
    if fs != 4 or not relay:
        return [piece] + [swap(piece, "fs", fs, mask) for mask in range(1, fs)]
    far = swap(piece, "fs", 4, 2)
    near = swap(piece, "fs", 4, 1)
    middle = lax.ppermute(piece, "fs", [(1, 2), (2, 1)])
    relayed = lax.ppermute(far, "fs", [(1, 0), (2, 3)])
    me = lax.axis_index("fs")
    last = jnp.where((me == 1) | (me == 2), middle, relayed)
    return [piece, near, far, last]


def gather_weight(shard, cut_axis, fs, relay=False):
    half = shard.shape[cut_axis] // 2
    group = lax.axis_index("grp")
    mine = lax.dynamic_slice_in_dim(shard, group * half, half, cut_axis)
    other = lax.dynamic_slice_in_dim(shard, (1 - group) * half, half, cut_axis)
    firsts = over_fs(mine, fs, relay)
    seconds = [other] + [
        lax.ppermute(firsts[mask], "grp", [(0, 1), (1, 0)]) for mask in range(1, fs)
    ]
    return firsts, seconds


def halves_swapped(value, axis):
    half = value.shape[axis] // 2
    group = lax.axis_index("grp")
    return jnp.concatenate(
        [
            lax.dynamic_slice_in_dim(value, group * half, half, axis),
            lax.dynamic_slice_in_dim(value, (1 - group) * half, half, axis),
        ],
        axis=axis,
    )


def gather_rows(piece, tp):
    blocks = [None] * tp
    blocks[0] = piece
    bit = tp // 2
    while bit:
        for at in range(tp):
            if blocks[at] is not None and not at & bit and blocks[at | bit] is None:
                blocks[at | bit] = "due"
        for at in range(tp):
            if isinstance(blocks[at], str):
                blocks[at] = swap(blocks[at ^ bit], "tp", tp, bit)
        bit //= 2
    return blocks


def normed_blocks(blocks, gain, fs, tp):
    feature_count = gain.shape[0]
    width, fine = feature_count // tp, feature_count // fs
    squares = sum(
        jnp.sum(jnp.square(block.astype(jnp.float32)), axis=1) for block in blocks
    )
    inverse = lax.rsqrt(squares / feature_count + 1e-06)[:, None]
    stacked = jnp.stack(blocks)
    me_fs, me_tp = lax.axis_index("fs"), lax.axis_index("tp")
    pieces = []
    for mask in range(fs):
        block = me_fs ^ mask
        first = block * fine
        whole = lax.dynamic_index_in_dim(stacked, (first // width) ^ me_tp, 0, keepdims=False)
        if fine != width:
            whole = lax.dynamic_slice_in_dim(whole, first % width, fine, 1)
        gain_piece = lax.dynamic_slice_in_dim(gain, first, fine, 0)
        pieces.append((whole.astype(jnp.float32) * inverse * gain_piece).astype(jnp.bfloat16))
    return jnp.concatenate(pieces, axis=1)


def scatter_sum(terms, fs, tp):
    stacked = jnp.stack(terms)
    ratio = fs // tp
    me_fs, me_tp = lax.axis_index("fs"), lax.axis_index("tp")
    sums = []
    for mask in range(tp):
        parts = [
            lax.dynamic_index_in_dim(
                stacked, ((me_tp ^ mask) * ratio + at) ^ me_fs, 0, keepdims=False
            )
            for at in range(ratio)
        ]
        sums.append(parts[0] if ratio == 1 else jnp.concatenate(parts, axis=1))
    bit = 1
    while bit < tp:
        kept = {}
        for at in range(tp):
            if sums[at] is not None and not at & bit:
                got = swap(sums[at | bit].astype(jnp.bfloat16), "tp", tp, bit)
                kept[at] = sums[at].astype(jnp.float32) + got.astype(jnp.float32)
        sums = [kept.get(at) for at in range(tp)]
        bit *= 2
    return sums[0]


def make(fs, tp):
    def layer(
        tokens,
        norm1_gain,
        weight_u,
        weight_v,
        scale_u,
        scale_v,
        mix_gain,
        spatial_weight,
        spatial_bias,
        weight_out,
        scale_out,
        norm2_gain,
        weight_up,
        scale_up,
        weight_down,
        scale_down,
    ):
        half = weight_u.shape[1] // 2
        token_blocks = gather_rows(tokens, tp)
        both = jnp.stack([weight_u, weight_v], axis=1).astype(jnp.bfloat16)
        both_mine, both_other = gather_weight(both, 2, fs)
        scales = jnp.stack([scale_out, scale_down])
        all_scales = [scales] + [swap(scales, "fs", fs, mask) for mask in range(1, fs)]
        out_mine, out_other = gather_weight(weight_out.astype(jnp.bfloat16), 0, fs)
        up_mine, up_other = gather_weight(weight_up.astype(jnp.bfloat16), 1, fs, relay=True)
        down_mine, down_other = gather_weight(weight_down.astype(jnp.bfloat16), 0, fs, relay=True)

        normed_in = normed_blocks(token_blocks, norm1_gain, fs, tp)
        full_u = jnp.concatenate(
            [jnp.concatenate([a[:, 0], b[:, 0]], axis=1) for a, b in zip(both_mine, both_other)]
        )
        full_v = jnp.concatenate(
            [jnp.concatenate([a[:, 1], b[:, 1]], axis=1) for a, b in zip(both_mine, both_other)]
        )
        pre_v = jnp.dot(normed_in, full_v, preferred_element_type=jnp.float32)
        pre_u = jnp.dot(normed_in, full_u, preferred_element_type=jnp.float32)
        act_v = jax.nn.gelu(pre_v * halves_swapped(scale_v, 0))
        gate_u = jax.nn.gelu(pre_u * halves_swapped(scale_u, 0))
        local_width = 2 * half
        row_sums, row_squares = lax.psum(
            (jnp.sum(act_v, axis=1), jnp.sum(act_v * act_v, axis=1)), "tp"
        )
        row_mean = (row_sums / GM_W)[:, None]
        square = (row_squares / GM_W)[:, None]
        v_norm = (
            (act_v - row_mean)
            * lax.rsqrt(square - row_mean * row_mean + 1e-06)
            * halves_swapped(mix_gain, 0)
        ).astype(jnp.bfloat16)
        group_index = lax.axis_index("tp") * local_width // (GM_W // GROUPS)
        lower_mask = jnp.tril(jnp.ones((BLOCK, BLOCK), jnp.float32))
        spatial_mask = (
            lax.dynamic_index_in_dim(spatial_weight, group_index, 0, keepdims=False) * lower_mask
        ).astype(jnp.bfloat16)
        block_bias = lax.dynamic_index_in_dim(spatial_bias, group_index, 0, keepdims=False)
        blocks = v_norm.reshape(-1, BLOCK, local_width)
        mixed = jnp.einsum("ts,nsc->ntc", spatial_mask, blocks, preferred_element_type=jnp.float32)
        mixed = mixed + block_bias[None, :, None]
        gated = (gate_u * mixed.reshape(-1, local_width)).astype(jnp.bfloat16)

        terms = []
        for a, b, scale in zip(out_mine, out_other, all_scales):
            product = jnp.dot(gated, jnp.concatenate([a, b]), preferred_element_type=jnp.float32)
            terms.append((product * scale[0]).astype(jnp.bfloat16))
        mixer_sum = scatter_sum(terms, fs, tp)
        residual = (tokens.astype(jnp.float32) + mixer_sum).astype(jnp.bfloat16)

        normed_mid = normed_blocks(gather_rows(residual, tp), norm2_gain, fs, tp)
        full_up = jnp.concatenate(
            [jnp.concatenate([a, b], axis=1) for a, b in zip(up_mine, up_other)]
        )
        pre_up = jnp.dot(normed_mid, full_up, preferred_element_type=jnp.float32)
        hidden = jnp.square(jax.nn.relu(pre_up * halves_swapped(scale_up, 0))).astype(jnp.bfloat16)
        terms = []
        for a, b, scale in zip(down_mine, down_other, all_scales):
            product = jnp.dot(hidden, jnp.concatenate([a, b]), preferred_element_type=jnp.float32)
            terms.append((product * scale[1]).astype(jnp.bfloat16))
        channel_sum = scatter_sum(terms, fs, tp)
        return (residual.astype(jnp.float32) + channel_sum).astype(jnp.bfloat16)

    return layer


def solution(mesh):
    placed = (
        P(("grp", "fs"), "tp"),
        P(),
        P("fs", "tp"),
        P("fs", "tp"),
        P("tp"),
        P("tp"),
        P("tp"),
        P(),
        P(),
        P("tp", "fs"),
        P("fs"),
        P(),
        P("fs", "tp"),
        P("tp"),
        P("tp", "fs"),
        P("fs"),
    )
    fs, tp = mesh.shape["fs"], mesh.shape["tp"]
    return jax.shard_map(
        make(fs, tp),
        mesh=mesh,
        in_specs=placed,
        out_specs=P(("grp", "fs"), "tp"),
        check_vma=False,
    )
```

```python
import jax
import jax.numpy as jnp
from jax import lax
from jax.sharding import PartitionSpec as P

GM_W = 1024
GROUPS = 4
BLOCK = 128


def swap(value, axis, size, mask):
    return lax.ppermute(value, axis, [(k, k ^ mask) for k in range(size)])


def over_fs(piece, fs, relay, near_too):
    if fs != 4 or not relay:
        return [piece] + [swap(piece, "fs", fs, mask) for mask in range(1, fs)]
    far = swap(piece, "fs", 4, 2)
    near = swap(piece, "fs", 4, 1) if near_too else None
    middle = lax.ppermute(piece, "fs", [(1, 2), (2, 1)])
    relayed = lax.ppermute(far, "fs", [(1, 0), (2, 3)])
    me = lax.axis_index("fs")
    last = jnp.where((me == 1) | (me == 2), middle, relayed)
    return [piece, near, far, last]


def gather_weight(shard, cut_axis, fs, relay=False, whole_near=False):
    half = shard.shape[cut_axis] // 2
    group = lax.axis_index("grp")
    mine = lax.dynamic_slice_in_dim(shard, group * half, half, cut_axis)
    other = lax.dynamic_slice_in_dim(shard, (1 - group) * half, half, cut_axis)
    whole_near = whole_near and relay and fs == 4
    firsts = over_fs(mine, fs, relay, not whole_near)
    if whole_near:
        near = swap(jnp.concatenate([mine, other], axis=cut_axis), "fs", fs, 1)
        firsts[1], near_other = jnp.split(near, 2, axis=cut_axis)
    seconds = [other] + [
        near_other
        if whole_near and mask == 1
        else lax.ppermute(firsts[mask], "grp", [(0, 1), (1, 0)])
        for mask in range(1, fs)
    ]
    return firsts, seconds


def halves_swapped(value, axis):
    half = value.shape[axis] // 2
    group = lax.axis_index("grp")
    return jnp.concatenate(
        [
            lax.dynamic_slice_in_dim(value, group * half, half, axis),
            lax.dynamic_slice_in_dim(value, (1 - group) * half, half, axis),
        ],
        axis=axis,
    )


def gather_rows(piece, tp):
    blocks = [None] * tp
    blocks[0] = piece
    bit = tp // 2
    while bit:
        for at in range(tp):
            if blocks[at] is not None and not at & bit and blocks[at | bit] is None:
                blocks[at | bit] = "due"
        for at in range(tp):
            if isinstance(blocks[at], str):
                blocks[at] = swap(blocks[at ^ bit], "tp", tp, bit)
        bit //= 2
    return blocks


def normed_blocks(blocks, gain, fs, tp):
    feature_count = gain.shape[0]
    width, fine = feature_count // tp, feature_count // fs
    squares = sum(
        jnp.sum(jnp.square(block.astype(jnp.float32)), axis=1) for block in blocks
    )
    inverse = lax.rsqrt(squares / feature_count + 1e-06)[:, None]
    stacked = jnp.stack(blocks)
    me_fs, me_tp = lax.axis_index("fs"), lax.axis_index("tp")
    pieces = []
    for mask in range(fs):
        block = me_fs ^ mask
        first = block * fine
        whole = lax.dynamic_index_in_dim(stacked, (first // width) ^ me_tp, 0, keepdims=False)
        if fine != width:
            whole = lax.dynamic_slice_in_dim(whole, first % width, fine, 1)
        gain_piece = lax.dynamic_slice_in_dim(gain, first, fine, 0)
        pieces.append((whole.astype(jnp.float32) * inverse * gain_piece).astype(jnp.bfloat16))
    return jnp.concatenate(pieces, axis=1)


def scatter_sum(terms, fs, tp):
    stacked = jnp.stack(terms)
    ratio = fs // tp
    me_fs, me_tp = lax.axis_index("fs"), lax.axis_index("tp")
    sums = []
    for mask in range(tp):
        parts = [
            lax.dynamic_index_in_dim(
                stacked, ((me_tp ^ mask) * ratio + at) ^ me_fs, 0, keepdims=False
            )
            for at in range(ratio)
        ]
        sums.append(parts[0] if ratio == 1 else jnp.concatenate(parts, axis=1))
    bit = 1
    while bit < tp:
        kept = {}
        for at in range(tp):
            if sums[at] is not None and not at & bit:
                got = swap(sums[at | bit].astype(jnp.bfloat16), "tp", tp, bit)
                kept[at] = sums[at].astype(jnp.float32) + got.astype(jnp.float32)
        sums = [kept.get(at) for at in range(tp)]
        bit *= 2
    return sums[0]


def make(fs, tp):
    def layer(
        tokens,
        norm1_gain,
        weight_u,
        weight_v,
        scale_u,
        scale_v,
        mix_gain,
        spatial_weight,
        spatial_bias,
        weight_out,
        scale_out,
        norm2_gain,
        weight_up,
        scale_up,
        weight_down,
        scale_down,
    ):
        half = weight_u.shape[1] // 2
        token_blocks = gather_rows(tokens, tp)
        both = jnp.stack([weight_u, weight_v], axis=1).astype(jnp.bfloat16)
        both_mine, both_other = gather_weight(both, 2, fs)
        scales = jnp.stack([scale_out, scale_down])
        all_scales = [scales] + [swap(scales, "fs", fs, mask) for mask in range(1, fs)]
        out_mine, out_other = gather_weight(weight_out.astype(jnp.bfloat16), 0, fs)
        up_mine, up_other = gather_weight(weight_up.astype(jnp.bfloat16), 1, fs, relay=True)
        down_mine, down_other = gather_weight(weight_down.astype(jnp.bfloat16), 0, fs, relay=True, whole_near=True)

        normed_in = normed_blocks(token_blocks, norm1_gain, fs, tp)
        full_u = jnp.concatenate(
            [jnp.concatenate([a[:, 0], b[:, 0]], axis=1) for a, b in zip(both_mine, both_other)]
        )
        full_v = jnp.concatenate(
            [jnp.concatenate([a[:, 1], b[:, 1]], axis=1) for a, b in zip(both_mine, both_other)]
        )
        pre_v = jnp.dot(normed_in, full_v, preferred_element_type=jnp.float32)
        pre_u = jnp.dot(normed_in, full_u, preferred_element_type=jnp.float32)
        act_v = jax.nn.gelu(pre_v * halves_swapped(scale_v, 0))
        gate_u = jax.nn.gelu(pre_u * halves_swapped(scale_u, 0))
        local_width = 2 * half
        row_sums, row_squares = lax.psum(
            (jnp.sum(act_v, axis=1), jnp.sum(act_v * act_v, axis=1)), "tp"
        )
        row_mean = (row_sums / GM_W)[:, None]
        square = (row_squares / GM_W)[:, None]
        v_norm = (
            (act_v - row_mean)
            * lax.rsqrt(square - row_mean * row_mean + 1e-06)
            * halves_swapped(mix_gain, 0)
        ).astype(jnp.bfloat16)
        group_index = lax.axis_index("tp") * local_width // (GM_W // GROUPS)
        lower_mask = jnp.tril(jnp.ones((BLOCK, BLOCK), jnp.float32))
        spatial_mask = (
            lax.dynamic_index_in_dim(spatial_weight, group_index, 0, keepdims=False) * lower_mask
        ).astype(jnp.bfloat16)
        block_bias = lax.dynamic_index_in_dim(spatial_bias, group_index, 0, keepdims=False)
        blocks = v_norm.reshape(-1, BLOCK, local_width)
        mixed = jnp.einsum("ts,nsc->ntc", spatial_mask, blocks, preferred_element_type=jnp.float32)
        mixed = mixed + block_bias[None, :, None]
        gated = (gate_u * mixed.reshape(-1, local_width)).astype(jnp.bfloat16)

        terms = []
        for a, b, scale in zip(out_mine, out_other, all_scales):
            product = jnp.dot(gated, jnp.concatenate([a, b]), preferred_element_type=jnp.float32)
            terms.append((product * scale[0]).astype(jnp.bfloat16))
        mixer_sum = scatter_sum(terms, fs, tp)
        residual = (tokens.astype(jnp.float32) + mixer_sum).astype(jnp.bfloat16)

        normed_mid = normed_blocks(gather_rows(residual, tp), norm2_gain, fs, tp)
        full_up = jnp.concatenate(
            [jnp.concatenate([a, b], axis=1) for a, b in zip(up_mine, up_other)]
        )
        pre_up = jnp.dot(normed_mid, full_up, preferred_element_type=jnp.float32)
        hidden = jnp.square(jax.nn.relu(pre_up * halves_swapped(scale_up, 0))).astype(jnp.bfloat16)
        terms = []
        for a, b, scale in zip(down_mine, down_other, all_scales):
            product = jnp.dot(hidden, jnp.concatenate([a, b]), preferred_element_type=jnp.float32)
            terms.append((product * scale[1]).astype(jnp.bfloat16))
        channel_sum = scatter_sum(terms, fs, tp)
        return (residual.astype(jnp.float32) + channel_sum).astype(jnp.bfloat16)

    return layer


def solution(mesh):
    placed = (
        P(("grp", "fs"), "tp"),
        P(),
        P("fs", "tp"),
        P("fs", "tp"),
        P("tp"),
        P("tp"),
        P("tp"),
        P(),
        P(),
        P("tp", "fs"),
        P("fs"),
        P(),
        P("fs", "tp"),
        P("tp"),
        P("tp", "fs"),
        P("fs"),
    )
    fs, tp = mesh.shape["fs"], mesh.shape["tp"]
    return jax.shard_map(
        make(fs, tp),
        mesh=mesh,
        in_specs=placed,
        out_specs=P(("grp", "fs"), "tp"),
        check_vma=False,
    )
```
